32 devices in a mesh: rep: 2 (over x), fs: 4 (over z), tp: 4 (over y, core).
Axes of the slice: x: 2, y: 2, z: 4, core: 2. Of those that a mesh axis runs over, the one named last changes fastest.
Arguments:
- tokens: bfloat16 [8, 1024, 2048], P(('rep', 'fs')), may hold values from -6 to 6
- mix_gain: bfloat16 [2048], replicated, may hold values from 0.099609375 to 1.8984375
- value_weight: bfloat16 [2048, 1024], P('fs', 'tp'), may hold values from -0.125 to 0.125
- gate_weight: bfloat16 [2048, 1024], P('fs', 'tp'), may hold values from -0.125 to 0.125
- mix_taps: bfloat16 [31, 1024], P(None, 'tp'), may hold values from -1 to 1
- head_gain: bfloat16 [1024], P('tp'), may hold values from 0.099609375 to 1.8984375
- out_weight: bfloat16 [1024, 2048], P('fs', 'tp'), may hold values from -0.1875 to 0.1875
- ffn_gain: bfloat16 [2048], replicated, may hold values from 0.099609375 to 1.8984375
- ffgate_weight: bfloat16 [2048, 6144], P('fs', 'tp'), may hold values from -0.125 to 0.125
- up_weight: bfloat16 [2048, 6144], P('fs', 'tp'), may hold values from -0.125 to 0.125
- ff_taps: bfloat16 [3, 6144], P(None, 'tp'), may hold values from -3.5 to 3.5
- down_weight: bfloat16 [2048, 6144], P('fs', 'tp'), may hold values from -0.078125 to 0.078125
Outputs:
- layer_out: bfloat16 [8, 1024, 2048], P(('rep', 'fs'), 'tp')
The draws below stay inside these ranges and needn't reach their ends.
All inputs are finite; a program needn't handle non-finite values.
Results may differ from the reference program's by a relative error of at most 0.01.
Values may be sent and summed in bfloat16 or wider, within the bound.
A program may use at most 128 MiB of HBM per device.

```python
import jax
import jax.numpy as jnp
from jax import lax

D = 2048
CW = 1024
FF = 6144
HEAD = 128
KW = 31
KF = 3
LEN = 1024
BATCH = 8


def steps_of(stream_key, shape, cuts, smallest, largest):
    level = 1.0
    for dim, parts in cuts:
        draws = jax.random.uniform(jax.random.fold_in(jax.random.fold_in(stream_key, 6), dim), (parts,), jnp.float32, smallest / len(cuts), largest / len(cuts))
        level = level * jnp.repeat(jnp.exp(draws), shape[dim] // parts).reshape((-1,) + (1,) * (len(shape) - 1 - dim))
    return level


def normal_values(stream_key, shape, scale, bound, pieces=(), kind=jnp.bfloat16):
    level = steps_of(stream_key, shape, pieces, -0.22, 0.18) if pieces else 1.0
    array = jax.random.normal(stream_key, shape, jnp.float32) * scale * level
    return jnp.minimum(jnp.maximum(array, -bound), bound).astype(kind)


def setup_inputs(seed: int = 0) -> dict:
    key_of = jax.random.split(jax.random.key(seed), 13)
    tokens = normal_values(key_of[0], (BATCH, LEN, D), 1.0, 6.0, ((0, 8),))
    mix_gain = jnp.clip(1.0 + 0.18 * jax.random.normal(key_of[1], (D,), jnp.float32), 0.099609375, 1.8984375).astype(jnp.bfloat16)
    value_weight = normal_values(key_of[2], (D, CW), D ** -0.5, 0.125, ((0, 4), (1, 4)))
    gate_weight = normal_values(key_of[3], (D, CW), D ** -0.5, 0.125, ((0, 4), (1, 4)))
    mix_taps = normal_values(key_of[4], (KW, CW), KW ** -0.5, 1.0, ((1, 4),))
    head_gain = jnp.clip(1.0 + 0.18 * jax.random.normal(key_of[5], (CW,), jnp.float32), 0.099609375, 1.8984375).astype(jnp.bfloat16)
    out_weight = normal_values(key_of[6], (CW, D), CW ** -0.5, 0.1875, ((0, 4), (1, 4)))
    ffn_gain = jnp.clip(1.0 + 0.18 * jax.random.normal(key_of[7], (D,), jnp.float32), 0.099609375, 1.8984375).astype(jnp.bfloat16)
    ffgate_weight = normal_values(key_of[8], (D, FF), D ** -0.5, 0.125, ((0, 4), (1, 4)))
    up_weight = normal_values(key_of[9], (D, FF), D ** -0.5, 0.125, ((0, 4), (1, 4)))
    ff_taps = normal_values(key_of[10], (KF, FF), KF ** -0.5, 3.5, ((1, 4),))
    down_weight = normal_values(key_of[11], (D, FF), FF ** -0.5, 0.078125, ((0, 4), (1, 4)))
    return {"tokens": tokens, "mix_gain": mix_gain, "value_weight": value_weight, "gate_weight": gate_weight, "mix_taps": mix_taps, "head_gain": head_gain, "out_weight": out_weight, "ffn_gain": ffn_gain, "ffgate_weight": ffgate_weight, "up_weight": up_weight, "ff_taps": ff_taps, "down_weight": down_weight}


norm_floor = 0.01

def row_norm(floats_in, scales):
    floats = floats_in.astype(jnp.float32)
    scaled = floats * lax.rsqrt(lax.optimization_barrier(jnp.mean(floats * floats, axis=-1, keepdims=True)) + norm_floor)
    return (scaled * scales.astype(jnp.float32)).astype(jnp.bfloat16)

def causal_conv(signal, kernel_taps):
    reach = kernel_taps.shape[0]
    length = signal.shape[0]
    padded = jnp.pad(signal, ((reach - 1, 0), (0, 0)))
    summed = padded[0:length] * kernel_taps[0]
    for offset in range(1, reach):
        summed = summed + padded[offset:offset + length] * kernel_taps[offset]
    return summed

def head_norm(signal, scales):
    length = signal.shape[0]
    grouped = signal.reshape(length, signal.shape[1] // HEAD, HEAD)
    centre = grouped - lax.optimization_barrier(jnp.mean(grouped, axis=-1, keepdims=True))
    spread = lax.optimization_barrier(jnp.mean(centre * centre, axis=-1, keepdims=True))
    normal = (centre * lax.rsqrt(spread + norm_floor)).reshape(signal.shape)
    return normal * scales.astype(jnp.float32)

def reference(tokens, mix_gain, value_weight, gate_weight, mix_taps, head_gain, out_weight, ffn_gain, ffgate_weight, up_weight, ff_taps, down_weight):

    def sublayers(sequence):
        normed = row_norm(sequence, mix_gain)
        values = jnp.dot(normed, value_weight, preferred_element_type=jnp.float32)
        gating = jnp.dot(normed, gate_weight, preferred_element_type=jnp.float32)
        glu_out = values * jax.nn.sigmoid(gating)
        mixed_pos = causal_conv(glu_out, mix_taps.astype(jnp.float32))
        head_out = jax.nn.silu(head_norm(mixed_pos, head_gain)).astype(jnp.bfloat16)
        hidden = (sequence.astype(jnp.float32) + jnp.dot(head_out, out_weight, preferred_element_type=jnp.float32)).astype(jnp.bfloat16)
        normed_ffn = row_norm(hidden, ffn_gain)
        ffgate = jnp.dot(normed_ffn, ffgate_weight, preferred_element_type=jnp.float32)
        ff_up = jnp.dot(normed_ffn, up_weight, preferred_element_type=jnp.float32)
        product = (jax.nn.silu(causal_conv(ffgate, ff_taps.astype(jnp.float32))) * ff_up).astype(jnp.bfloat16)
        down_sum = lax.dot_general(product, down_weight, (((1,), (1,)), ((), ())), preferred_element_type=jnp.float32)
        return (hidden.astype(jnp.float32) + down_sum).astype(jnp.bfloat16)
    return lax.map(sublayers, tokens)
```

```python
import jax
import jax.numpy as jnp
from jax import lax
from jax.sharding import PartitionSpec as P


HEAD = 128


norm_floor = 0.01


def row_norm(floats_in, scales):
    floats = floats_in.astype(jnp.float32)
    scaled = floats * lax.rsqrt(jnp.mean(floats * floats, axis=-1, keepdims=True) + norm_floor)
    return (scaled * scales.astype(jnp.float32)).astype(jnp.bfloat16)


def causal_conv(signal, kernel_taps):
    reach = kernel_taps.shape[0]
    length = signal.shape[0]
    padded = jnp.pad(signal, ((reach - 1, 0), (0, 0)))
    summed = padded[0:length] * kernel_taps[0]
    for offset in range(1, reach):
        summed = summed + padded[offset : offset + length] * kernel_taps[offset]
    return summed


def head_norm(signal, scales):
    heads = []
    for start in range(0, signal.shape[1], HEAD):
        part = signal[:, start : start + HEAD]
        centre = part - jnp.mean(part, axis=-1, keepdims=True)
        spread = jnp.mean(centre * centre, axis=-1, keepdims=True)
        gain = scales[start : start + HEAD].astype(jnp.float32)
        heads.append(jax.nn.silu(centre * lax.rsqrt(spread + norm_floor) * gain))
    return jnp.concatenate(heads, axis=1).astype(jnp.bfloat16)


def fits(rows):
    return lax.axis_size("fs") == 4 and lax.axis_size("rep") == 2 and rows % 32 == 0


def pieces_of(shard):
    n = lax.axis_size("fs")
    f, r = lax.axis_index("fs"), lax.axis_index("rep")
    half = shard.shape[0] // 2
    mine = lax.dynamic_slice_in_dim(shard, r * half, half, 0)
    far = lax.ppermute(mine, "fs", [(0, 2), (1, 3), (2, 0), (3, 1)])
    up = lax.ppermute(mine, "fs", [(0, 1), (1, 2), (2, 3)])
    down = lax.ppermute(mine, "fs", [(1, 0), (2, 1), (3, 2)])
    last = lax.ppermute(far, "fs", [(2, 3), (1, 0)])

    def swap(block, members):
        pairs = []
        for m in members:
            pairs += [(m, n + m), (n + m, m)]
        return lax.ppermute(block, ("rep", "fs"), pairs)

    far_x = swap(far, (0, 1, 2, 3))
    up_x, down_x = swap(up, (1, 2, 3)), swap(down, (0, 1, 2))
    last_x = swap(last, (0, 3))
    low, high = f == 0, f == n - 1
    before, before_x = jnp.where(low, last, up), jnp.where(low, last_x, up_x)
    after, after_x = jnp.where(high, last, down), jnp.where(high, last_x, down_x)
    o = 1 - r
    return [
        ((f + 2) % n, r, far),
        ((f + 2) % n, o, far_x),
        ((f + n - 1) % n, r, before),
        ((f + 1) % n, r, after),
        ((f + n - 1) % n, o, before_x),
        ((f + 1) % n, o, after_x),
    ]


def gather_rows(shard):
    if not fits(shard.shape[0]):
        return lax.all_gather(shard, "fs", axis=0, tiled=True)
    n = lax.axis_size("fs")
    rows = shard.shape[0]
    full = jnp.zeros((n * rows, shard.shape[1]), shard.dtype)
    full = lax.dynamic_update_slice_in_dim(full, shard, lax.axis_index("fs") * rows, 0)
    for s, h, block in pieces_of(shard):
        full = lax.dynamic_update_slice_in_dim(full, block, s * rows + h * (rows // 2), 0)
    return full


def gather_small(shard):
    if not fits(shard.shape[0]):
        return lax.all_gather(shard, "fs", axis=0, tiled=True)
    n = lax.axis_size("fs")
    f, r = lax.axis_index("fs"), lax.axis_index("rep")
    rows = shard.shape[0]
    half = rows // 2
    mine = lax.dynamic_slice_in_dim(shard, r * half, half, 0)
    full = jnp.zeros((n * rows, shard.shape[1]), shard.dtype)
    full = lax.dynamic_update_slice_in_dim(full, shard, f * rows, 0)
    swaps = [(m, (m + n) % (2 * n)) for m in range(2 * n)]
    for hop in range(1, n):
        pairs = [(m, (m + hop) % n) for m in range(n)]
        here = lax.ppermute(mine, "fs", pairs)
        there = lax.ppermute(here, ("rep", "fs"), swaps)
        base = (f + n - hop) % n * rows
        full = lax.dynamic_update_slice_in_dim(full, here, base + r * half, 0)
        full = lax.dynamic_update_slice_in_dim(full, there, base + (1 - r) * half, 0)
    return full


def tp_scatter(block):
    size = lax.axis_size("tp")
    if size != 4:
        return lax.psum_scatter(block, "tp", scatter_dimension=0, tiled=True)
    t = lax.axis_index("tp")
    y, c = t // 2, t % 2
    parts = block.reshape(2, 2, block.shape[0] // size, block.shape[1])
    theirs = lax.dynamic_index_in_dim(parts, 1 - c, 1, keepdims=False)
    mine = lax.dynamic_index_in_dim(parts, c, 1, keepdims=False)
    got = lax.ppermute(theirs, "tp", [(0, 1), (1, 0), (2, 3), (3, 2)])

    def row_of(i):
        a = lax.dynamic_index_in_dim(mine, i, 0, keepdims=False).astype(jnp.float32)
        return a + lax.dynamic_index_in_dim(got, i, 0, keepdims=False).astype(jnp.float32)

    away = row_of(1 - y).astype(jnp.bfloat16)
    other = lax.ppermute(away, "tp", [(0, 2), (2, 0), (1, 3), (3, 1)])
    return row_of(y) + other.astype(jnp.float32)


def down_sums(product, shard, spread):
    n = lax.axis_size("fs")
    f, r = lax.axis_index("fs"), lax.axis_index("rep")
    rows = shard.shape[0]
    half = rows // 2

    def partial(weights):
        return lax.dot_general(
            product, weights, (((1,), (1,)), ((), ())), preferred_element_type=jnp.float32
        ).astype(jnp.bfloat16)

    early = partial(jnp.concatenate([shard] + [block for _, _, block in spread[:2]], axis=0))
    late = partial(jnp.concatenate([block for _, _, block in spread[2:]], axis=0))
    early, late = tp_scatter(early), tp_scatter(late)
    own = early[:, :rows]
    parts = [late[:, i * half : (i + 1) * half] for i in range(4)]

    def in_order(a, b):
        return jnp.concatenate([jnp.where(r == 0, a, b), jnp.where(r == 0, b, a)], axis=1)

    far = in_order(early[:, rows : rows + half], early[:, rows + half : 2 * rows])
    blocks = [own, in_order(parts[1], parts[3]), far, in_order(parts[0], parts[2])]
    return jnp.concatenate(
        [lax.select_n((s + n - f) % n, *blocks) for s in range(n)], axis=1
    )


def on_device(
    tokens,
    mix_gain,
    value_weight,
    gate_weight,
    mix_taps,
    head_gain,
    out_weight,
    ffn_gain,
    ffgate_weight,
    up_weight,
    ff_taps,
    down_weight,
):
    sequence = tokens[0]
    width = value_weight.shape[1]
    pair_full = gather_small(jnp.concatenate([value_weight, gate_weight], axis=1))
    out_full = lax.all_gather(out_weight, "fs", axis=0, tiled=True)
    normed = row_norm(sequence, mix_gain)
    both = jnp.dot(normed, pair_full, preferred_element_type=jnp.float32)
    glu_out = both[:, :width] * jax.nn.sigmoid(both[:, width:])
    mixed_pos = causal_conv(glu_out, mix_taps.astype(jnp.float32))
    head_out = head_norm(mixed_pos, head_gain)
    out_cols = out_full.shape[1]
    all_heads = lax.all_gather(head_out, "tp", axis=1, tiled=True)
    own_cols = lax.dynamic_slice_in_dim(sequence, lax.axis_index("tp") * out_cols, out_cols, 1)
    mixer_sum = jnp.dot(all_heads, out_full, preferred_element_type=jnp.float32)
    hidden_cols = (own_cols.astype(jnp.float32) + mixer_sum).astype(jnp.bfloat16)
    full_rows = lax.all_gather(hidden_cols, "tp", axis=1, tiled=True)
    normed_ffn = row_norm(full_rows, ffn_gain)
    gate_all = gather_rows(ffgate_weight)
    up_all = gather_rows(up_weight)
    ffgate = jnp.dot(normed_ffn, gate_all, preferred_element_type=jnp.float32)
    gated = jax.nn.silu(causal_conv(ffgate, ff_taps.astype(jnp.float32)))
    ff_up = jnp.dot(normed_ffn, up_all, preferred_element_type=jnp.float32)
    product = lax.optimization_barrier((gated * ff_up).astype(jnp.bfloat16))
    own_count = sequence.shape[0] // lax.axis_size("tp")
    own_rows = lax.dynamic_slice_in_dim(full_rows, lax.axis_index("tp") * own_count, own_count, 0)
    if fits(down_weight.shape[0]):
        spread = pieces_of(down_weight)
        result = down_sums(product, down_weight, spread)
    else:
        down_full = lax.all_gather(down_weight, "fs", axis=0, tiled=True)
        partial = lax.dot_general(
            product, down_full, (((1,), (1,)), ((), ())), preferred_element_type=jnp.float32
        )
        result = lax.psum_scatter(
            partial.astype(jnp.bfloat16), "tp", scatter_dimension=0, tiled=True
        )
    return (own_rows.astype(jnp.float32) + result.astype(jnp.float32)).astype(jnp.bfloat16)[None]


def solution(mesh):
    placed = (
        P(("rep", "fs"), None, None),
        P(),
        P("fs", "tp"),
        P("fs", "tp"),
        P(None, "tp"),
        P("tp"),
        P("fs", "tp"),
        P(),
        P("fs", "tp"),
        P("fs", "tp"),
        P(None, "tp"),
        P("fs", "tp"),
    )

    return jax.shard_map(
        on_device,
        mesh=mesh,
        in_specs=placed,
        out_specs=P(("rep", "fs"), "tp", None),
        check_vma=False,
    )
```
